32 devices in a mesh: sp: 16 (over z, y, x), tp: 2 (over core).
Axes of the slice: x: 2, y: 2, z: 4, core: 2. Of those that a mesh axis runs over, the one named last changes fastest.
Arguments:
- queries: bfloat16 [4096, 1024], P('sp', 'tp'), may hold values from -6 to 6
- keys: bfloat16 [4096, 256], P('sp', 'tp'), may hold values from -6 to 6
- values: bfloat16 [4096, 256], P('sp', 'tp'), may hold values from -24 to 24
- sink_logit: float32 [16], P('tp'), may hold values from 3 to 7
- w_out: bfloat16 [1024, 2048], replicated, may hold values from -0.1875 to 0.1875
- residual: bfloat16 [4096, 2048], P(('sp', 'tp')), may hold values from -3 to 3
- norm_gain: float32 [2048], replicated, may hold values from 0.1 to 1.9
- w_gate: bfloat16 [16, 2048, 2048], P('sp', None, 'tp'), may hold values from -0.5 to 0.5
- w_up: bfloat16 [16, 2048, 2048], P('sp', None, 'tp'), may hold values from -0.5 to 0.5
- w_down: bfloat16 [16, 2048, 2048], P('sp', 'tp'), may hold values from -0.125 to 0.125
- expert_ids: int32 [4096, 2], P(('sp', 'tp')), may hold values from 0 to 15, all different within a row; in each aligned block of 128 rows (0 to 127, 128 to 255, ...) at most 24 rows name the same one
- route_weight: float32 [4096, 2], P(('sp', 'tp')), may hold values from 0.2 to 1
Outputs:
- final: bfloat16 [4096, 2048], P(('sp', 'tp'))
The draws below stay inside these ranges and needn't reach their ends.
Inputs may be any that keep to these rules, and one draw needn't show every extreme that they name: `expert_ids`: in the rows of one device each row names 2 different experts and no expert is named by more than 24 rows; some expert is named by exactly 24 of them.
All inputs are finite; a program needn't handle non-finite values.
Results may differ from the reference program's by a relative error of at most 0.0097.
Values may be sent and summed in bfloat16 or wider, within the bound.
No kernel may reach another device: no remote copies, remote signals or barrier semaphores. Data moves between devices by JAX's collectives and lax.ppermute only.
A program may use at most 128 MiB of HBM per device.

```python
import math
import jax
import jax.numpy as jnp
import numpy as np
from jax import lax

D = 2048
HEADS = 16
KV_HEADS = 4
HEAD_DIM = 64
FF = 2048
WINDOW = 128
TOPK = 2
SPAN = 256
EXPERTS = 16
CAP = 24
SEQ = 4096
N_TP = 2


def draw_queries(key, part):
    noise_draw = jnp.clip(jax.random.normal(jax.random.fold_in(key, 1), (SEQ, KV_HEADS, HEADS // KV_HEADS, HEAD_DIM), jnp.float32), -4.0, 4.0)
    return noise_draw.reshape(SEQ, HEADS * HEAD_DIM).astype(jnp.bfloat16)


def draw_keys(key, part):
    noise_draw = jnp.clip(jax.random.normal(jax.random.fold_in(key, 2), (SEQ, KV_HEADS, 1, HEAD_DIM), jnp.float32), -4.0, 4.0)
    return noise_draw.reshape(SEQ, KV_HEADS * HEAD_DIM).astype(jnp.bfloat16)


def expert_matrix(key):
    weight_scale = D ** (-0.5)
    drawn = weight_scale * jax.random.normal(key, (EXPERTS, D, FF), jnp.float32)
    return jnp.clip(drawn, -0.5, 0.5).astype(jnp.bfloat16)


def draw_w_gate(key, part):
    return expert_matrix(jax.random.fold_in(key, 11))


def draw_w_up(key, part):
    return expert_matrix(jax.random.fold_in(key, 13))


def levels(rng, dims, cuts, least, largest):
    level = 1.0
    for axis_at, shards_of in cuts:
        steps = jax.random.uniform(jax.random.fold_in(jax.random.fold_in(rng, 6), axis_at), (shards_of,), jnp.float32, least / len(cuts), largest / len(cuts))
        level = level * jnp.repeat(jnp.exp(steps), dims[axis_at] // shards_of).reshape((-1,) + (1,) * (len(dims) - 1 - axis_at))
    return level


def deal_out(stream_key, own, number, rows, number_of, top, bound, lean):
    sequence = jax.random.permutation(stream_key, number_of)
    packed, usual = load_shares(number_of, rows * top, bound, lean, True), load_shares(number_of, rows * top, bound, lean, False)
    places = jnp.arange(number_of)

    def named(sizes, rotation):
        used = int((sizes > 0).sum())
        fixed = max(1, used // 4)
        shifted = fixed + (places - fixed + rotation * (used - fixed)) % max(1, number_of - fixed)
        return jnp.zeros((number_of,), jnp.int32).at[sequence[jnp.where(places < fixed, places, shifted)]].set(jnp.asarray(sizes, jnp.int32))

    sizes = jnp.where(number % 4 == 0, named(packed, number // 4), named(usual, number - number // 4 - 1))
    mixed = jax.random.permutation(jax.random.fold_in(own, 3), number_of)
    source_of, taker = mixed[0:number_of // 2 * 2:2], mixed[1:number_of // 2 * 2:2]
    margin = jnp.minimum(sizes[source_of] - 1, bound - sizes[taker]) // 2
    margin = jnp.where((source_of == sequence[0]) | (taker == sequence[0]) | (sizes[taker] == 0), 0, jnp.maximum(margin, 0))
    shifted = jax.random.randint(jax.random.fold_in(own, 4), (number_of // 2,), 0, 1 << 20) % (margin + 1)
    sizes = sizes.at[source_of].add(-shifted).at[taker].add(shifted)
    items = jnp.searchsorted(jnp.cumsum(sizes), jnp.arange(rows * top), side="right").astype(jnp.int32)
    table = items.reshape(top, rows).T
    table = table[jax.random.permutation(jax.random.fold_in(own, 1), rows)]
    rotation = jax.random.randint(jax.random.fold_in(own, 2), (rows, 1), 0, top)
    return jnp.take_along_axis(table, (jnp.arange(top)[None, :] + rotation) % top, axis=1)


def load_shares(number_of, total, reach, slope, full):
    portions = [(1 << 20) // math.isqrt(rank ** slope) + 1 for rank in range(1, number_of + 1)]
    largest = reach if full else min(reach, max(-(-total // number_of), total * portions[0] // sum(portions)))
    least = 1 if total - largest >= number_of - 1 else 0
    holding, surplus = [largest] + [least] * (number_of - 1), total - largest - least * (number_of - 1)
    while surplus > 0:
        movable = [i for i in range(1, number_of) if holding[i] < largest] or [i for i in range(1, number_of) if holding[i] < reach]
        mass, left = sum([portions[i] for i in movable]), surplus
        for i in movable:
            extra = min(reach - holding[i], max(1, left * portions[i] // mass), surplus)
            holding[i] = holding[i] + extra
            surplus = surplus - extra
    return np.array(holding)


def normal_values(key, dims, spread, reach, shards=(), kind=jnp.bfloat16):
    level = levels(key, dims, shards, -0.22, 0.18) if shards else 1.0
    array = jax.random.normal(key, dims, jnp.float32) * spread * level
    return jnp.minimum(jnp.maximum(array, -reach), reach).astype(kind)


def setup_inputs(seed: int = 0) -> dict:
    splits = jax.random.split(jax.random.key(seed), 13)
    queries = draw_queries(jax.random.fold_in(splits[12], 71), 0)
    keys = draw_keys(jax.random.fold_in(splits[12], 71), 0)
    values = normal_values(splits[2], (SEQ, KV_HEADS * HEAD_DIM), 4.0, 24.0, ((0, 16), (1, 2)))
    sink_logit = jnp.clip(3.0 + 4.0 * jax.random.uniform(splits[3], (HEADS,), jnp.float32) ** levels(splits[3], (HEADS,), ((0, 2),), -0.2, 0.2), 3.0, 7.0)
    w_out = normal_values(splits[4], (HEADS * HEAD_DIM, D), (HEADS * HEAD_DIM) ** -0.5, 0.1875)
    residual = normal_values(splits[5], (SEQ, D), 0.5, 3.0, ((0, 32),))
    norm_gain = jnp.clip(1.0 + 0.18 * jax.random.normal(splits[6], (D,), jnp.float32), 0.1, 1.9)
    w_gate = draw_w_gate(jax.random.fold_in(splits[12], 71), 0)
    w_up = draw_w_up(jax.random.fold_in(splits[12], 71), 0)
    w_down = normal_values(splits[9], (EXPERTS, FF, D), FF ** -0.5, 0.125, ((0, 16), (1, 2)))
    expert_ids_keys = jax.random.split(jax.random.fold_in(splits[10], 1), SEQ // (SPAN // N_TP))
    expert_ids_turns = jax.random.permutation(jax.random.fold_in(splits[10], 3), SEQ // (SPAN // N_TP))
    expert_ids = jax.vmap(lambda own, number: deal_out(jax.random.fold_in(splits[10], 2), own, number, SPAN // N_TP, EXPERTS, TOPK, CAP, 2))(expert_ids_keys, expert_ids_turns).reshape((SEQ, TOPK))
    route_weight = jnp.clip(0.2 + 0.8 * jax.random.uniform(splits[11], (SEQ, TOPK), jnp.float32) ** levels(splits[11], (SEQ, TOPK), ((0, 32),), -0.2, 0.2), 0.2, 1.0)
    return dict(queries=queries, keys=keys, values=values, sink_logit=sink_logit, w_out=w_out, residual=residual, norm_gain=norm_gain, w_gate=w_gate, w_up=w_up, w_down=w_down, expert_ids=expert_ids, route_weight=route_weight)


CLAMP_LIMIT = 7.0
GATE_ALPHA = 1.702
EPSILON = 1e-06
NEG_BIG = -1e+30
SORT_ROWS = 128

def reference(queries, keys, values, sink_logit, w_out, residual, norm_gain, w_gate, w_up, w_down, expert_ids, route_weight):
    seq_len = queries.shape[0]
    repeat = HEADS // KV_HEADS
    block_count = seq_len // SPAN
    keys_pad = jnp.pad(keys, ((WINDOW, WINDOW), (0, 0))).reshape(seq_len + 2 * WINDOW, KV_HEADS, HEAD_DIM)
    values_pad = jnp.pad(values, ((WINDOW, WINDOW), (0, 0))).reshape(seq_len + 2 * WINDOW, KV_HEADS, HEAD_DIM)
    query_blocks = queries.reshape(block_count, SPAN, KV_HEADS, repeat, HEAD_DIM)
    logit_sink = sink_logit.astype(jnp.float32).reshape(KV_HEADS, repeat)[:, :, None, None]

    def attend_block(inputs):
        query_block, block_index = inputs
        row_start = block_index * SPAN
        key_block = lax.dynamic_slice_in_dim(keys_pad, row_start, SPAN + 2 * WINDOW, 0)
        value_block = lax.dynamic_slice_in_dim(values_pad, row_start, SPAN + 2 * WINDOW, 0)
        scores = jnp.einsum('qgrd,kgd->grqk', query_block.astype(jnp.float32), key_block.astype(jnp.float32)) * HEAD_DIM ** (-0.5)
        query_pos = row_start + jnp.arange(SPAN, dtype=jnp.int32)
        key_pos = row_start - WINDOW + jnp.arange(SPAN + 2 * WINDOW, dtype=jnp.int32)
        key_gap = key_pos[None, :] - query_pos[:, None]
        in_window = (jnp.abs(key_gap) <= WINDOW) & (key_pos[None, :] >= 0) & (key_pos[None, :] < seq_len)
        scores = jnp.where(in_window, scores, NEG_BIG)
        peak = jnp.maximum(lax.optimization_barrier(jnp.max(scores, axis=-1, keepdims=True)), logit_sink)
        expo = jnp.exp(scores - peak)
        divisor = lax.optimization_barrier(jnp.sum(expo, axis=-1, keepdims=True)) + jnp.exp(logit_sink - peak)
        softmax_w = (expo / divisor).astype(jnp.bfloat16)
        mixed = jnp.einsum('grqk,kgd->qgrd', softmax_w.astype(jnp.float32), value_block.astype(jnp.float32))
        return mixed.reshape(SPAN, HEADS * HEAD_DIM).astype(jnp.bfloat16)
    attended = lax.map(attend_block, (query_blocks, jnp.arange(block_count, dtype=jnp.int32)))
    attended = attended.reshape(seq_len, HEADS * HEAD_DIM)
    attn_proj = lax.optimization_barrier(jnp.dot(attended, w_out, preferred_element_type=jnp.float32).astype(jnp.bfloat16))
    midway = residual.astype(jnp.float32) + attn_proj.astype(jnp.float32)
    normed = (midway * lax.rsqrt(lax.optimization_barrier(jnp.mean(midway * midway, axis=-1, keepdims=True)) + EPSILON) * norm_gain).astype(jnp.bfloat16)
    assigned = expert_ids.reshape(-1).astype(jnp.int32)
    count_all = assigned.shape[0]
    sort_order = jnp.argsort(assigned, stable=True).astype(jnp.int32)
    sorted_expert = assigned[sort_order]
    counts = lax.optimization_barrier(jnp.sum((assigned[:, None] == jnp.arange(EXPERTS, dtype=jnp.int32)[None, :]).astype(jnp.int32), axis=0))
    filled = (counts + SORT_ROWS - 1) // SORT_ROWS * SORT_ROWS
    pad_ends = jnp.cumsum(filled).astype(jnp.int32)
    pad_starts = pad_ends - filled
    plain_starts = (jnp.cumsum(counts) - counts).astype(jnp.int32)
    slot_of = (pad_starts[sorted_expert] + jnp.arange(count_all, dtype=jnp.int32) - plain_starts[sorted_expert]).astype(jnp.int32)
    slot_total = count_all + EXPERTS * SORT_ROWS
    block_total = slot_total // SORT_ROWS
    slot_token = jnp.zeros((slot_total,), jnp.int32).at[slot_of].set(sort_order // TOPK)
    block_expert = jnp.minimum(jnp.searchsorted(pad_ends, jnp.arange(block_total, dtype=jnp.int32) * SORT_ROWS, side='right'), EXPERTS - 1).astype(jnp.int32)
    inputs = normed[slot_token].reshape(block_total, SORT_ROWS, D)
    half_width = FF // N_TP

    def expert_block(pair_in):
        rows_in, expert = pair_in
        gate_pre = jnp.dot(rows_in, w_gate[expert], preferred_element_type=jnp.float32)
        up_pre = jnp.dot(rows_in, w_up[expert], preferred_element_type=jnp.float32)
        act_clip = jnp.minimum(gate_pre, CLAMP_LIMIT)
        up_clip = jnp.clip(up_pre, -CLAMP_LIMIT, CLAMP_LIMIT)
        hidden = ((up_clip + 1.0) * act_clip * jax.nn.sigmoid(GATE_ALPHA * act_clip)).astype(jnp.bfloat16)
        down_full = w_down[expert]
        summed = jnp.zeros((rows_in.shape[0], D), jnp.float32)
        for half in range(N_TP):
            down_part = jnp.dot(hidden[:, half * half_width:(half + 1) * half_width], down_full[half * half_width:(half + 1) * half_width], preferred_element_type=jnp.float32)
            summed = summed + down_part.astype(jnp.bfloat16).astype(jnp.float32)
        return summed.astype(jnp.bfloat16)
    slot_out = lax.map(expert_block, (inputs, block_expert)).reshape(slot_total, D)
    assign_slot = jnp.zeros((count_all,), jnp.int32).at[sort_order].set(slot_of)
    picked = slot_out[assign_slot].reshape(seq_len, TOPK, D)
    routed = lax.optimization_barrier(jnp.sum(picked.astype(jnp.float32) * route_weight[:, :, None], axis=1))
    return (midway + routed).astype(jnp.bfloat16)
```

```python
import jax
import jax.numpy as jnp
from jax import lax
from jax.sharding import PartitionSpec as P

HEAD_DIM = 64
WINDOW = 128


CLAMP_LIMIT = 7.0
GATE_ALPHA = 1.702
EPSILON = 1e-06
NEG_BIG = -1e30


def with_halo(shard, sides, width):
    for axis, dim in sides:
        devices, length = (lax.axis_size(axis), shard.shape[dim])
        up = [(i, (i + 1) % devices) for i in range(devices - 1)]
        down = [(j, i) for i, j in up]
        last = lax.slice_in_dim(shard, length - width, length, axis=dim)
        leading = lax.slice_in_dim(shard, 0, width, axis=dim)
        before = lax.ppermute(last, axis, up)
        after = lax.ppermute(leading, axis, down)
        shard = jnp.concatenate([before, shard, after], axis=dim)
    return shard


OUT_CHUNKS = 1


def attend(queries, keys, values, sink_logit, first_pos, seq_total, groups):
    rows = queries.shape[0]
    local_heads = queries.shape[1] // HEAD_DIM
    repeat = local_heads // groups
    key_rows = keys.shape[0]
    logit_sink = sink_logit.reshape(groups, repeat)[:, :, None, None]
    query_block = queries.reshape(rows, groups, repeat, HEAD_DIM)
    key_block = keys.reshape(key_rows, groups, HEAD_DIM)
    value_block = values.reshape(key_rows, groups, HEAD_DIM)
    scores = jnp.einsum(
        "qgrd,kgd->grqk", query_block, key_block, preferred_element_type=jnp.float32
    ) * HEAD_DIM ** (-0.5)
    query_at = jnp.arange(rows, dtype=jnp.int32)
    key_at = jnp.arange(key_rows, dtype=jnp.int32) - WINDOW
    key_pos = first_pos + key_at
    in_window = (
        (jnp.abs(key_at[None, :] - query_at[:, None]) <= WINDOW)
        & (key_pos[None, :] >= 0)
        & (key_pos[None, :] < seq_total)
    )
    scores = jnp.where(in_window, scores, NEG_BIG)
    peak = jnp.maximum(jnp.max(scores, axis=-1, keepdims=True), logit_sink)
    expo = jnp.exp(scores - peak)
    divisor = jnp.sum(expo, axis=-1, keepdims=True) + jnp.exp(logit_sink - peak)
    softmax_w = (expo / divisor).astype(jnp.bfloat16)
    mixed = jnp.einsum("grqk,kgd->qgrd", softmax_w, value_block, preferred_element_type=jnp.float32)
    return mixed.reshape(rows, local_heads * HEAD_DIM).astype(jnp.bfloat16)


def swap_pair(array):
    count = lax.axis_size("tp")
    return lax.ppermute(array, "tp", [(i, (i + 1) % count) for i in range(count)])


def exchange(rows):
    count = lax.axis_size("sp")
    boxes = rows.reshape(count, rows.shape[0] // count, rows.shape[1])
    return lax.all_to_all(boxes, "sp", split_axis=0, concat_axis=0, tiled=True).reshape(rows.shape)


def slot_tables(ids, weights, expert_count, capacity):
    flat = ids.reshape(-1)
    onehot = (flat[:, None] == jnp.arange(expert_count, dtype=jnp.int32)[None, :]).astype(jnp.int32)
    earlier = jnp.cumsum(onehot, axis=0) - onehot
    rank = jnp.sum(earlier * onehot, axis=1).reshape(ids.shape)
    slots = ids * capacity + rank
    numbers = jnp.arange(expert_count * capacity, dtype=jnp.int32)
    table = jnp.any(slots[None, :, :] == numbers[:, None, None], axis=2).astype(jnp.bfloat16)
    mix = jnp.sum(
        jnp.where(slots[:, :, None] == numbers[None, None, :], weights[:, :, None], 0.0), axis=1
    ).astype(jnp.bfloat16)
    return table, mix


def pick(table, rows):
    return jnp.dot(table, rows, preferred_element_type=jnp.float32).astype(jnp.bfloat16)


def gated(gate_pre, up_pre):
    act_clip = jnp.minimum(gate_pre, CLAMP_LIMIT)
    up_clip = jnp.clip(up_pre, -CLAMP_LIMIT, CLAMP_LIMIT)
    return ((up_clip + 1.0) * act_clip * jax.nn.sigmoid(GATE_ALPHA * act_clip)).astype(jnp.bfloat16)


def project(chunks, weight):
    width = weight.shape[0] // len(chunks)
    total = None
    for at, chunk in enumerate(chunks):
        part = jnp.dot(
            chunk, weight[at * width : (at + 1) * width], preferred_element_type=jnp.float32
        )
        total = part if total is None else total + part
    return total


def expert_halves(chunks, w_gate, w_up, w_down, out_chunks):
    others = [swap_pair(chunk) for chunk in chunks]
    hidden_mine = gated(project(chunks, w_gate), project(chunks, w_up))
    hidden_other = gated(project(others, w_gate), project(others, w_up))
    width = w_down.shape[1] // out_chunks
    results = []
    for at in range(out_chunks):
        weight = w_down[:, at * width : (at + 1) * width]
        part_other = jnp.dot(hidden_other, weight, preferred_element_type=jnp.float32)
        back = swap_pair(part_other.astype(jnp.bfloat16))
        part = jnp.dot(hidden_mine, weight, preferred_element_type=jnp.float32)
        part = part.astype(jnp.bfloat16).astype(jnp.float32) + back.astype(jnp.float32)
        results.append(part.astype(jnp.bfloat16))
    return results


def per_device(
    queries,
    keys,
    values,
    sink_logit,
    w_out,
    residual,
    norm_gain,
    w_gate,
    w_up,
    w_down,
    expert_ids,
    route_weight,
):
    span_rows = queries.shape[0]
    sp_size = lax.axis_size("sp")
    tp_at = lax.axis_index("tp")
    pair_size = lax.axis_size("tp")
    own_count = span_rows // pair_size
    offset = lax.axis_index("sp") * span_rows
    expert_count = w_gate.shape[0] * sp_size
    top_count = expert_ids.shape[1]
    capacity = 3 * own_count * top_count // (2 * expert_count)

    padded = with_halo(jnp.stack([keys, values]), (("sp", 1),), WINDOW)
    groups = keys.shape[1] // HEAD_DIM

    def rows_of(side):
        first = side * own_count
        block = lax.dynamic_slice_in_dim(queries, first, own_count, 0)
        window = lax.dynamic_slice_in_dim(padded, first, own_count + 2 * WINDOW, 1)
        return attend(
            block, window[0], window[1], sink_logit, offset + first, span_rows * sp_size, groups
        )

    received = swap_pair(rows_of(1 - tp_at))
    mine = rows_of(tp_at)
    attended = jnp.where(
        tp_at == 0,
        jnp.concatenate([mine, received], axis=1),
        jnp.concatenate([received, mine], axis=1),
    )
    attn_proj = jnp.dot(attended, w_out, preferred_element_type=jnp.float32).astype(jnp.bfloat16)
    midway = residual.astype(jnp.float32) + attn_proj.astype(jnp.float32)
    normed = (
        midway * lax.rsqrt(jnp.mean(midway * midway, axis=-1, keepdims=True) + EPSILON) * norm_gain
    ).astype(jnp.bfloat16)

    table, mix = slot_tables(expert_ids, route_weight, expert_count, capacity)
    rows_in = exchange(pick(table, normed))
    results = expert_halves([rows_in], w_gate[0], w_up[0], w_down[0], OUT_CHUNKS)
    sums = [jnp.dot(mix, exchange(part), preferred_element_type=jnp.float32) for part in results]
    routed = jnp.concatenate(sums, axis=1)
    return (midway + routed).astype(jnp.bfloat16)


def solution(mesh):
    in_specs = (
        P("sp", "tp"),
        P("sp", "tp"),
        P("sp", "tp"),
        P("tp"),
        P(),
        P(("sp", "tp"), None),
        P(),
        P("sp", None, "tp"),
        P("sp", None, "tp"),
        P("sp", "tp", None),
        P(("sp", "tp"), None),
        P(("sp", "tp"), None),
    )
    out_specs = P(("sp", "tp"), None)
    return jax.shard_map(
        per_device, mesh=mesh, in_specs=in_specs, out_specs=out_specs, check_vma=False
    )
```

```python
import jax
import jax.numpy as jnp
from jax import lax
from jax.sharding import PartitionSpec as P

HEAD_DIM = 64
WINDOW = 128


CLAMP_LIMIT = 7.0
GATE_ALPHA = 1.702
EPSILON = 1e-06
NEG_BIG = -1e30


def with_halo(shard, sides, width):
    for axis, dim in sides:
        devices, length = (lax.axis_size(axis), shard.shape[dim])
        up = [(i, (i + 1) % devices) for i in range(devices - 1)]
        down = [(j, i) for i, j in up]
        last = lax.slice_in_dim(shard, length - width, length, axis=dim)
        leading = lax.slice_in_dim(shard, 0, width, axis=dim)
        before = lax.ppermute(last, axis, up)
        after = lax.ppermute(leading, axis, down)
        shard = jnp.concatenate([before, shard, after], axis=dim)
    return shard


IN_CHUNKS = 1
OUT_CHUNKS = 1


def attend(queries, keys, values, sink_logit, first_pos, seq_total, groups):
    rows = queries.shape[0]
    local_heads = queries.shape[1] // HEAD_DIM
    repeat = local_heads // groups
    key_rows = keys.shape[0]
    logit_sink = sink_logit.reshape(groups, repeat)[:, :, None, None]
    query_block = queries.reshape(rows, groups, repeat, HEAD_DIM)
    key_block = keys.reshape(key_rows, groups, HEAD_DIM)
    value_block = values.reshape(key_rows, groups, HEAD_DIM)
    scores = jnp.einsum(
        "qgrd,kgd->grqk", query_block, key_block, preferred_element_type=jnp.float32
    ) * HEAD_DIM ** (-0.5)
    query_at = jnp.arange(rows, dtype=jnp.int32)
    key_at = jnp.arange(key_rows, dtype=jnp.int32) - WINDOW
    key_pos = first_pos + key_at
    in_window = (
        (jnp.abs(key_at[None, :] - query_at[:, None]) <= WINDOW)
        & (key_pos[None, :] >= 0)
        & (key_pos[None, :] < seq_total)
    )
    scores = jnp.where(in_window, scores, NEG_BIG)
    peak = jnp.maximum(jnp.max(scores, axis=-1, keepdims=True), logit_sink)
    expo = jnp.exp(scores - peak)
    divisor = jnp.sum(expo, axis=-1, keepdims=True) + jnp.exp(logit_sink - peak)
    softmax_w = (expo / divisor).astype(jnp.bfloat16)
    mixed = jnp.einsum("grqk,kgd->qgrd", softmax_w, value_block, preferred_element_type=jnp.float32)
    return mixed.reshape(rows, local_heads * HEAD_DIM).astype(jnp.bfloat16)


def swap_pair(array):
    count = lax.axis_size("tp")
    return lax.ppermute(array, "tp", [(i, (i + 1) % count) for i in range(count)])


def exchange(rows):
    count = lax.axis_size("sp")
    boxes = rows.reshape(count, rows.shape[0] // count, rows.shape[1])
    return lax.all_to_all(boxes, "sp", split_axis=0, concat_axis=0, tiled=True).reshape(rows.shape)


def slot_tables(ids, weights, expert_count, capacity):
    flat = ids.reshape(-1)
    onehot = (flat[:, None] == jnp.arange(expert_count, dtype=jnp.int32)[None, :]).astype(jnp.int32)
    earlier = jnp.cumsum(onehot, axis=0) - onehot
    rank = jnp.sum(earlier * onehot, axis=1).reshape(ids.shape)
    slots = ids * capacity + rank
    numbers = jnp.arange(expert_count * capacity, dtype=jnp.int32)
    table = jnp.any(slots[None, :, :] == numbers[:, None, None], axis=2).astype(jnp.bfloat16)
    mix = jnp.sum(
        jnp.where(slots[:, :, None] == numbers[None, None, :], weights[:, :, None], 0.0), axis=1
    ).astype(jnp.bfloat16)
    return table, mix


def pick(table, rows):
    return jnp.dot(table, rows, preferred_element_type=jnp.float32).astype(jnp.bfloat16)


def gated(gate_pre, up_pre):
    act_clip = jnp.minimum(gate_pre, CLAMP_LIMIT)
    up_clip = jnp.clip(up_pre, -CLAMP_LIMIT, CLAMP_LIMIT)
    return ((up_clip + 1.0) * act_clip * jax.nn.sigmoid(GATE_ALPHA * act_clip)).astype(jnp.bfloat16)


def project(chunks, weight):
    width = weight.shape[0] // len(chunks)
    total = None
    for at, chunk in enumerate(chunks):
        part = jnp.dot(
            chunk, weight[at * width : (at + 1) * width], preferred_element_type=jnp.float32
        )
        total = part if total is None else total + part
    return total


def expert_halves(chunks, w_gate, w_up, w_down, out_chunks):
    count = chunks[0].shape[0]
    both = [jnp.concatenate([chunk, swap_pair(chunk)], axis=0) for chunk in chunks]
    hidden = gated(project(both, w_gate), project(both, w_up))
    width = w_down.shape[1] // out_chunks
    results = []
    for at in range(out_chunks):
        weight = w_down[:, at * width : (at + 1) * width]
        part = jnp.dot(hidden, weight, preferred_element_type=jnp.float32).astype(jnp.bfloat16)
        back = swap_pair(part[count:])
        total = part[:count].astype(jnp.float32) + back.astype(jnp.float32)
        results.append(total.astype(jnp.bfloat16))
    return results


def per_device(
    queries,
    keys,
    values,
    sink_logit,
    w_out,
    residual,
    norm_gain,
    w_gate,
    w_up,
    w_down,
    expert_ids,
    route_weight,
):
    span_rows = queries.shape[0]
    sp_size = lax.axis_size("sp")
    tp_at = lax.axis_index("tp")
    pair_size = lax.axis_size("tp")
    own_count = span_rows // pair_size
    offset = lax.axis_index("sp") * span_rows
    expert_count = w_gate.shape[0] * sp_size
    top_count = expert_ids.shape[1]
    capacity = 3 * own_count * top_count // (2 * expert_count)

    padded = with_halo(jnp.stack([keys, values]), (("sp", 1),), WINDOW)
    groups = keys.shape[1] // HEAD_DIM

    def rows_of(side):
        first = side * own_count
        block = lax.dynamic_slice_in_dim(queries, first, own_count, 0)
        window = lax.dynamic_slice_in_dim(padded, first, own_count + 2 * WINDOW, 1)
        return attend(
            block, window[0], window[1], sink_logit, offset + first, span_rows * sp_size, groups
        )

    received = swap_pair(rows_of(1 - tp_at))
    mine = rows_of(tp_at)
    attended = jnp.where(
        tp_at == 0,
        jnp.concatenate([mine, received], axis=1),
        jnp.concatenate([received, mine], axis=1),
    )
    attn_proj = jnp.dot(attended, w_out, preferred_element_type=jnp.float32).astype(jnp.bfloat16)
    midway = residual.astype(jnp.float32) + attn_proj.astype(jnp.float32)
    normed = (
        midway * lax.rsqrt(jnp.mean(midway * midway, axis=-1, keepdims=True) + EPSILON) * norm_gain
    ).astype(jnp.bfloat16)

    table, mix = slot_tables(expert_ids, route_weight, expert_count, capacity)
    width = normed.shape[1] // IN_CHUNKS
    rows_in = [
        exchange(pick(table, normed[:, at * width : (at + 1) * width])) for at in range(IN_CHUNKS)
    ]
    results = expert_halves(rows_in, w_gate[0], w_up[0], w_down[0], OUT_CHUNKS)
    sums = [jnp.dot(mix, exchange(part), preferred_element_type=jnp.float32) for part in results]
    routed = jnp.concatenate(sums, axis=1)
    return (midway + routed).astype(jnp.bfloat16)


def solution(mesh):
    in_specs = (
        P("sp", "tp"),
        P("sp", "tp"),
        P("sp", "tp"),
        P("tp"),
        P(),
        P(("sp", "tp"), None),
        P(),
        P("sp", None, "tp"),
        P("sp", None, "tp"),
        P("sp", "tp", None),
        P(("sp", "tp"), None),
        P(("sp", "tp"), None),
    )
    out_specs = P(("sp", "tp"), None)
    return jax.shard_map(
        per_device, mesh=mesh, in_specs=in_specs, out_specs=out_specs, check_vma=False
    )
```
